1024 devices in a mesh: pp: 32 (over z), fs: 4 (over y), tp: 8 (over x, core).
Axes of the slice: x: 4, y: 4, z: 32, core: 2. Of those that a mesh axis runs over, the one named last changes fastest.
Arguments:
- tokens_in: bfloat16 [32, 32, 8, 2048], P('pp', ('fs', 'tp')), may hold values from -6 to 6
- weight_in: bfloat16 [32, 2048, 512], P('pp'), may hold values from -0.125 to 0.125
- conv_taps: float32 [32, 4, 512], P('pp'), may hold values from -3 to 3
- conv_bias: float32 [32, 512], P('pp'), may hold values from -2 to 2
- gate_rate: bfloat16 [32, 8, 64, 64], P('pp'), may hold values from -0.75 to 0.75
- bias_rate: float32 [32, 512], P('pp'), may hold values from -3 to 3
- gate_input: bfloat16 [32, 8, 64, 64], P('pp'), may hold values from -0.75 to 0.75
- bias_input: float32 [32, 512], P('pp'), may hold values from -3 to 3
- decay_param: float32 [32, 512], P('pp'), may hold values from 3.5 to 7.5
- weight_out: bfloat16 [32, 512, 2048], P('pp'), may hold values from -0.5 to 0.5
- norm_gain: float32 [32, 2048], P('pp'), may hold values from 0.1 to 1.9
- norm_shift: float32 [32, 2048], P('pp'), may hold values from -2 to 2
Outputs:
- tokens_out: bfloat16 [32, 32, 8, 2048], P('pp', ('fs', 'tp'))
The draws below stay inside these ranges and needn't reach their ends.
All inputs are finite; a program needn't handle non-finite values.
Results may differ from the reference program's by a relative error of at most 0.022.
Values may be sent and summed in bfloat16 or wider, within the bound.
No kernel may reach another device: no remote copies, remote signals or barrier semaphores. Data moves between devices by JAX's collectives and lax.ppermute only.
A program may use at most 128 MiB of HBM per device.

```python
import jax
import jax.numpy as jnp
from jax import lax

D = 2048
LRU_W = 512
LRU_BLOCKS = 8
BLOCK_W = 64
CONV = 4
LEN = 8
SECTIONS = 32
SEQS = 32


def shard_levels(stream_key, shape, pieces, least, largest):
    def one(axis_at, shards_of):
        draws = jax.random.uniform(jax.random.fold_in(jax.random.fold_in(stream_key, 6), axis_at), (shards_of,), jnp.float32, least / len(pieces), largest / len(pieces))
        return jnp.repeat(jnp.exp(draws), shape[axis_at] // shards_of).reshape((-1,) + (1,) * (len(shape) - axis_at - 1))

    gain = one(*pieces[0])
    for cut in pieces[1:]:
        gain = gain * one(*cut)
    return gain


def centred(stream_key, shape, spread, bound, pieces=(), kind=jnp.bfloat16):
    factor_of = shard_levels(stream_key, shape, pieces, -0.22, 0.18) if pieces else 1.0
    entries = jax.random.normal(stream_key, shape, jnp.float32) * spread * factor_of
    return jnp.minimum(jnp.maximum(entries, -bound), bound).astype(kind)


def setup_inputs(seed: int = 0) -> dict:
    streams_of = jax.random.split(jax.random.key(seed), 13)
    tokens_in = centred(streams_of[0], (SECTIONS, SEQS, LEN, D), 1.0, 6.0, ((0, 32), (1, 32)))
    weight_in = centred(streams_of[1], (SECTIONS, D, LRU_W), D ** -0.5, 0.125, ((0, 32),))
    conv_taps = centred(streams_of[2], (SECTIONS, CONV, LRU_W), 0.5, 3.0, ((0, 32),), jnp.float32)
    conv_bias = centred(streams_of[3], (SECTIONS, LRU_W), 0.3, 2.0, ((0, 32),), jnp.float32)
    gate_rate = centred(streams_of[4], (SECTIONS, LRU_BLOCKS, BLOCK_W, BLOCK_W), BLOCK_W ** -0.5, 0.75, ((0, 32),))
    bias_rate = centred(streams_of[5], (SECTIONS, LRU_W), 0.5, 3.0, ((0, 32),), jnp.float32)
    gate_input = centred(streams_of[6], (SECTIONS, LRU_BLOCKS, BLOCK_W, BLOCK_W), BLOCK_W ** -0.5, 0.75, ((0, 32),))
    bias_input = centred(streams_of[7], (SECTIONS, LRU_W), 0.5, 3.0, ((0, 32),), jnp.float32)
    decay_param = jnp.clip(3.5 + 4.0 * jax.random.uniform(streams_of[8], (SECTIONS, LRU_W), jnp.float32) ** shard_levels(streams_of[8], (SECTIONS, LRU_W), ((0, 32),), -0.2, 0.2), 3.5, 7.5)
    weight_out = centred(streams_of[9], (SECTIONS, LRU_W, D), (LRU_W // 4) ** -0.5, 0.5, ((0, 32),))
    norm_gain = jnp.clip(1.0 + 0.18 * jax.random.normal(streams_of[10], (SECTIONS, D), jnp.float32), 0.1, 1.9)
    norm_shift = centred(streams_of[11], (SECTIONS, D), 0.3, 2.0, ((0, 32),), jnp.float32)
    return dict(tokens_in=tokens_in, weight_in=weight_in, conv_taps=conv_taps, conv_bias=conv_bias, gate_rate=gate_rate, bias_rate=bias_rate, gate_input=gate_input, bias_input=bias_input, decay_param=decay_param, weight_out=weight_out, norm_gain=norm_gain, norm_shift=norm_shift)


decay_scale = 8.0
norm_eps = 1e-05

def combine_steps(earlier, later):
    return (earlier[0] * later[0], later[0] * earlier[1] + later[1])

def recurrence(projected, conv_taps, conv_bias, gate_rate, bias_rate, gate_input, bias_input, decay_param):
    seq_count, length, channels = projected.shape
    tap_count = conv_taps.shape[0]
    padded = jnp.pad(projected.astype(jnp.float32), ((0, 0), (tap_count - 1, 0), (0, 0)))
    convolved = conv_bias + padded[:, 0:length] * conv_taps[0]
    for tap_index in range(1, tap_count):
        convolved = convolved + padded[:, tap_index:tap_index + length] * conv_taps[tap_index]
    convolved = convolved.astype(jnp.bfloat16)
    blocks = gate_rate.shape[0]
    block_width = gate_rate.shape[1]
    grouped = convolved.astype(jnp.float32).reshape(seq_count, length, blocks, block_width)
    rate_pre = jnp.einsum('bsnc,ncd->bsnd', grouped, gate_rate.astype(jnp.float32))
    input_pre = jnp.einsum('bsnc,ncd->bsnd', grouped, gate_input.astype(jnp.float32))
    rate_gate = jax.nn.sigmoid(rate_pre.reshape(seq_count, length, channels) + bias_rate)
    input_gate = jax.nn.sigmoid(input_pre.reshape(seq_count, length, channels) + bias_input)
    log_decay = -decay_scale * rate_gate * jax.nn.softplus(-decay_param)
    scale_in = jnp.sqrt(-jnp.expm1(2.0 * log_decay))
    driven = scale_in * input_gate * convolved.astype(jnp.float32)
    decay_now = jnp.exp(log_decay)
    unused, hidden = lax.associative_scan(combine_steps, (decay_now, driven), axis=1)
    return hidden.astype(jnp.bfloat16)

def finish(stream_rows, mixed_rows, weight_out, norm_gain, norm_shift):
    summed = stream_rows.astype(jnp.float32) + jnp.dot(mixed_rows, weight_out, preferred_element_type=jnp.float32)
    mean_value = lax.optimization_barrier(jnp.mean(summed, axis=-1, keepdims=True))
    centered = summed - mean_value
    variance = lax.optimization_barrier(jnp.mean(centered * centered, axis=-1, keepdims=True))
    return (centered * lax.rsqrt(variance + norm_eps) * norm_gain + norm_shift).astype(jnp.bfloat16)

def reference(tokens_in, weight_in, conv_taps, conv_bias, gate_rate, bias_rate, gate_input, bias_input, decay_param, weight_out, norm_gain, norm_shift):
    length = tokens_in.shape[2]
    model_width = tokens_in.shape[3]
    stream = tokens_in.reshape(-1, length, model_width)
    seq_count = stream.shape[0]

    def apply_section(current, section_weights):
        w_project, taps_now, cbias_now, grate_now, brate_now, ginput_now, binput_now, dparam_now, w_back, gain_now, shift_now = section_weights
        lru_width = w_project.shape[1]
        flat_rows = current.reshape(seq_count * length, model_width)
        projected = jnp.dot(flat_rows, w_project, preferred_element_type=jnp.float32).astype(jnp.bfloat16)
        projected = projected.reshape(seq_count, length, lru_width)
        mixed_out = recurrence(projected, taps_now, cbias_now, grate_now, brate_now, ginput_now, binput_now, dparam_now)
        result = finish(flat_rows, mixed_out.reshape(seq_count * length, lru_width), w_back, gain_now, shift_now)
        return (result.reshape(seq_count, length, model_width), None)
    stream, unused = lax.scan(apply_section, stream, (weight_in, conv_taps, conv_bias, gate_rate, bias_rate, gate_input, bias_input, decay_param, weight_out, norm_gain, norm_shift))
    return stream.reshape(tokens_in.shape)
```

```python
import functools

import jax
import jax.numpy as jnp
from jax import lax
from jax.experimental import pallas as pl
from jax.experimental.pallas import tpu as pltpu
from jax.sharding import PartitionSpec as P

decay_scale = 8.0
norm_eps = 1e-05

pair_stages = 4
group_count = 4
taps = 4


def stages_of(planes):
    paired = 2 * pair_stages
    return pair_stages + (planes - paired) // 4


def plane_of(stage, group, side):
    if stage < pair_stages:
        return 2 * stage + side
    return 2 * pair_stages + 4 * (stage - pair_stages) + 2 * (group % 2) + side


def section(x, weights, vector, at):
    rows, width = x.shape
    length = at.shape[1]
    count = rows // length
    parts, _, chans = weights.shape
    depth = width // parts
    half = chans // 2
    proj = jnp.dot(x[:, :depth], weights[0, :depth, :], preferred_element_type=jnp.float32)
    for t in range(1, parts):
        proj = proj + jnp.dot(
            x[:, t * depth : (t + 1) * depth],
            weights[t, :depth, :],
            preferred_element_type=jnp.float32,
        )
    proj = proj.astype(jnp.bfloat16).astype(jnp.float32).reshape(count, length, chans)
    conv = vector[taps : taps + 1][None] + proj * vector[taps - 1 : taps][None]
    for back in range(1, taps):
        moved = jnp.where(at >= back, pltpu.roll(proj, back, axis=1), 0.0)
        conv = conv + moved * vector[taps - 1 - back : taps - back][None]
    flat = conv.astype(jnp.bfloat16).reshape(rows, chans)
    rate, gate = [], []
    for h in range(2):
        maps = jnp.concatenate(
            [weights[t, 2 * depth :, :] for t in range(h * parts // 2, (h + 1) * parts // 2)], axis=0
        )
        both = jnp.dot(
            flat[:, h * half : (h + 1) * half], maps, preferred_element_type=jnp.float32
        )
        rate.append(both[:, :half])
        gate.append(both[:, half:])
    rate = jnp.concatenate(rate, axis=1) + vector[5:6]
    gate = jnp.concatenate(gate, axis=1) + vector[6:7]
    rate = 1.0 / (1.0 + jnp.exp(-rate))
    gate = 1.0 / (1.0 + jnp.exp(-gate))
    log_decay = rate * vector[7:8]
    lost = 1.0 + log_decay * (1.0 / 7.0)
    for k in (6.0, 5.0, 4.0, 3.0, 2.0):
        lost = 1.0 + log_decay * (1.0 / k) * lost
    lost = lost * log_decay
    hidden = jnp.sqrt(-lost * (2.0 + lost)) * gate * flat.astype(jnp.float32)
    decay = (1.0 + lost).reshape(count, length, chans)
    hidden = hidden.reshape(count, length, chans)
    back = 1
    while back < length:
        hidden = hidden + decay * jnp.where(at >= back, pltpu.roll(hidden, back, axis=1), 0.0)
        if 2 * back < length:
            decay = decay * jnp.where(at >= back, pltpu.roll(decay, back, axis=1), 1.0)
        back = 2 * back
    mixed = hidden.astype(jnp.bfloat16).reshape(rows, chans)
    update = [
        jnp.dot(mixed[:, :half], weights[t, depth : 2 * depth, :half], preferred_element_type=jnp.float32)
        + jnp.dot(mixed[:, half:], weights[t, depth : 2 * depth, half:], preferred_element_type=jnp.float32)
        for t in range(parts)
    ]
    summed = x.astype(jnp.float32) + jnp.concatenate(update, axis=1)
    mean_value = jnp.mean(summed, axis=1, keepdims=True)
    centered = summed - mean_value
    variance = jnp.mean(centered * centered, axis=1, keepdims=True)
    lines = width // chans
    gain = jnp.concatenate([vector[8 + q : 9 + q] for q in range(lines)], axis=1)
    shift = jnp.concatenate([vector[8 + lines + q : 9 + lines + q] for q in range(lines)], axis=1)
    normed = centered * lax.rsqrt(variance + norm_eps) * gain + shift
    return normed.astype(jnp.bfloat16)


def stage_kernel(step, length, both, enters, *refs):
    x_ref, own_ref, own_vectors = refs[:3]
    o_ref = refs[-1]
    plane = lax.axis_index("pp")
    paired = 2 * pair_stages
    mine = lax.div(lax.rem(plane, 4), 2)
    in_pair = plane < paired
    stage = jnp.where(in_pair, lax.div(plane, 2), pair_stages + lax.div(plane - paired, 4))
    group = step - 2 * stage
    active = (group >= 0) & (group < group_count)
    active = active & (in_pair | (lax.rem(group + 2 * group_count, 2) == mine))
    first = jnp.where(in_pair, 2 * mine, 0)
    last = jnp.where(active, jnp.where(in_pair, 2 * mine + 2, 4), first)
    if enters:
        o_ref[...] = jnp.where(plane < 2, refs[-2][...], x_ref[...])
    else:
        o_ref[...] = x_ref[...]
    rows = x_ref.shape[0]
    chans = own_vectors.shape[2]
    at = lax.broadcasted_iota(jnp.int32, (rows // length, length, chans), 1)

    def run(weights, vectors, j):
        o_ref[...] = section(o_ref[...], weights.at[:, j], vectors[j], at)

    def one(j, unused):
        if not both:
            run(own_ref, own_vectors, lax.rem(j, 2))
            return unused

        @pl.when(lax.div(j, 2) == mine)
        def _():
            run(own_ref, own_vectors, lax.rem(j, 2))

        @pl.when(lax.div(j, 2) != mine)
        def _():
            run(refs[3], refs[4], lax.rem(j, 2))

        return unused

    lax.fori_loop(first, last, one, 0)


def run_stage(step, length, x, entry, own, other):
    operands = (x,) + own + (other if other is not None else ()) + (() if entry is None else (entry,))
    rows, width = x.shape
    chans = own[1].shape[2]
    sections = 2 if other is None else 4
    spec = pl.BlockSpec(memory_space=pltpu.VMEM)
    return pl.pallas_call(
        functools.partial(stage_kernel, step, length, other is not None, entry is not None),
        out_shape=jax.ShapeDtypeStruct(x.shape, x.dtype),
        in_specs=[spec] * len(operands),
        out_specs=spec,
        compiler_params=pltpu.CompilerParams(vmem_limit_bytes=24 << 20),
        cost_estimate=pl.CostEstimate(
            flops=4 * sections * rows * width * chans,
            bytes_accessed=sections * 4 * width * chans,
            transcendentals=sections * 5 * rows * chans,
        ),
        name="stage",
    )(*operands)


def join_kernel(mine_ref, near_ref, o_ref, done):
    odd = lax.rem(lax.axis_index("pp"), 2)
    copies = [
        pltpu.make_async_copy(mine_ref, o_ref.at[:, odd], done.at[0]),
        pltpu.make_async_copy(near_ref, o_ref.at[:, 1 - odd], done.at[1]),
    ]
    for copy in copies:
        copy.start()
    for copy in copies:
        copy.wait()


def joined(mine, near):
    parts, lines, chans = mine.shape
    return pl.pallas_call(
        join_kernel,
        out_shape=jax.ShapeDtypeStruct((parts, 2, lines, chans), mine.dtype),
        in_specs=[pl.BlockSpec(memory_space=pl.ANY)] * 2,
        out_specs=pl.BlockSpec(memory_space=pltpu.VMEM),
        scratch_shapes=[pltpu.SemaphoreType.DMA((2,))],
        compiler_params=pltpu.CompilerParams(vmem_limit_bytes=12 << 20),
        name="join",
    )(mine, near)


def packed_weights(w_project, w_back, gate_rate, gate_input, parts):
    width, chans = w_project.shape
    depth, half, block = width // parts, chans // 2, gate_rate.shape[1]
    project = w_project.reshape(parts, depth, chans)
    back = w_back.reshape(2, half, parts, depth).transpose(2, 1, 0, 3).reshape(parts, half, 2 * depth)
    place = jnp.arange(parts)[:, None] % (parts // 2) == jnp.arange(parts // 2)[None, :]
    maps = jnp.stack([gate_rate, gate_input], axis=2)[:, :, :, None, :]
    maps = jnp.where(place[:, None, None, :, None], maps, jnp.zeros((), maps.dtype))
    return jnp.concatenate([project, back, maps.reshape(parts, block, chans)], axis=1)


def packed_shard(w_project, w_back, gate_rate, gate_input, parts):
    width, chans = w_project.shape
    depth, half, block = width // parts, chans // 2, gate_rate.shape[1]
    part = lax.axis_index("tp")
    project = lax.dynamic_slice_in_dim(w_project, part * depth, depth, 0)
    back = lax.dynamic_slice_in_dim(w_back, part * depth, depth, 1)
    back = jnp.concatenate([back[:half], back[half:]], axis=1)
    maps = [lax.dynamic_index_in_dim(g, part, 0, keepdims=False) for g in (gate_rate, gate_input)]
    place = (jnp.arange(half) // block) == part % (parts // 2)
    maps = [jnp.where(place, jnp.tile(g, (1, half // block)), jnp.zeros((), g.dtype)) for g in maps]
    return jnp.concatenate([project, back, jnp.concatenate(maps, axis=1)], axis=0)


def shards(
    tokens_in,
    weight_in,
    conv_taps,
    conv_bias,
    gate_rate,
    bias_rate,
    gate_input,
    bias_input,
    decay_param,
    weight_out,
    norm_gain,
    norm_shift,
):
    planes = lax.axis_size("pp")
    parts = lax.axis_size("tp")
    splits = lax.axis_size("fs")
    plane = lax.axis_index("pp")
    length, width = tokens_in.shape[2:]
    chans = weight_in.shape[2]
    odd = plane % 2
    paired = 2 * pair_stages

    def moved(x, pairs):
        return lax.ppermute(x, "pp", [(int(a), int(b)) for a, b in pairs])

    def in_order(mine, theirs):
        return jnp.stack(
            [jnp.where(odd == 0, mine, theirs), jnp.where(odd == 0, theirs, mine)], axis=0
        )

    packed = packed_weights(weight_in[0], weight_out[0], gate_rate[0], gate_input[0], parts)
    shard = packed_shard(weight_in[0], weight_out[0], gate_rate[0], gate_input[0], parts)
    swap = [(i, i ^ 1) for i in range(planes)]
    shard_near = moved(shard, swap)
    vector = jnp.concatenate(
        [
            conv_taps[0],
            conv_bias,
            bias_rate,
            bias_input,
            -decay_scale * jax.nn.softplus(-decay_param),
            norm_gain.reshape(-1, chans),
            norm_shift.reshape(-1, chans),
        ],
        axis=0,
    )
    vector_near = moved(vector, swap)
    near = lax.all_gather(shard_near, "tp", axis=0)
    own_vectors = in_order(vector, vector_near)

    across = [(i, i ^ 2) for i in range(paired, planes)]
    couple = in_order(shard, shard_near)
    lines = shard.shape[0] // splits
    piece = lax.dynamic_slice_in_dim(couple, lax.axis_index("fs") * lines, lines, 1)
    piece = moved(piece, across)
    other_vectors = moved(own_vectors, across)

    token = tokens_in.reshape(length, width)
    span = planes // group_count
    per = span // 2
    bases = [(g, s) for g in range(group_count) for s in range(2)]
    collected = jnp.concatenate(
        [token]
        + [moved(token, [(span * g + s + 2 * q, span * g + s) for g, s in bases]) for q in range(1, per)],
        axis=0,
    )
    entries = [collected] + [
        moved(collected, [(span * g + s, s) for s in range(2)]) for g in range(1, group_count)
    ]

    packed, collected, entries[1], piece, other_vectors, near = lax.optimization_barrier(
        (packed, collected, entries[1], piece, other_vectors, near)
    )
    entries[0] = collected
    own = joined(packed, near)
    other = lax.all_gather(piece, "fs", axis=1, tiled=True)

    stages = stages_of(planes)
    outputs, arrived = [], []
    for step in range(2 * stages + group_count - 2):
        x = arrived[step - 2] if step >= 2 else None
        entry = entries[step] if step < group_count else None
        if x is None:
            x, entry = entry, None
        if step == 1:
            x = lax.optimization_barrier((x, outputs[0]))[0]
        late = step >= 2 * pair_stages
        y = run_stage(
            step, length, x, entry, (own, own_vectors), (other, other_vectors) if late else None
        )
        pairs = [
            (plane_of(i, step - 2 * i, s), plane_of(i + 1, step - 2 * i, s))
            for i in range(stages - 1)
            if 0 <= step - 2 * i < group_count
            for s in range(2)
        ]
        if step == 2:
            other = lax.optimization_barrier((other, outputs[1], y))[0]
            other = lax.all_gather(other, "tp", axis=0)
        arrived.append(moved(y, pairs) if pairs else None)
        outputs.append(y)

    last = stages - 1
    stay = [plane_of(last, group_count - 1, s) for s in range(2)]
    done = outputs[-1]
    early = None
    parts_in = [
        moved(outputs[2 * last + g], [(plane_of(last, g, s), span * g + s) for s in range(2)])
        for g in range(group_count - 1)
    ]
    parts_in, done = lax.optimization_barrier((parts_in, done))
    for part in parts_in:
        early = part if early is None else early + part
    at_end = plane >= stay[0]
    done = jnp.where(at_end, done, early).reshape(per, length, width)
    final = None
    for c in range(1, per):
        send = jnp.where(at_end, done[c - 1], done[c])
        pairs = [
            (span * g + s, span * g + s + 2 * c) for g in range(group_count - 1) for s in range(2)
        ] + [(stay[s], span * (group_count - 1) + s + 2 * (c - 1)) for s in range(2)]
        part = moved(send, pairs)
        final = part if final is None else final + part
    keeps = at_end | ((plane % span < 2) & (plane < span * (group_count - 1)))
    final = jnp.where(keeps, jnp.where(at_end, done[per - 1], done[0]), final)
    return final.reshape(1, 1, length, width)


def solution(mesh):
    placed = (
        P("pp", ("fs", "tp"), None, None),
        P("pp", None, None),
        P("pp", None, None),
        P("pp", None),
        P("pp", None, None, None),
        P("pp", None),
        P("pp", None, None, None),
        P("pp", None),
        P("pp", None),
        P("pp", None, None),
        P("pp", None),
        P("pp", None),
    )
    return jax.shard_map(
        shards,
        mesh=mesh,
        in_specs=placed,
        out_specs=P("pp", ("fs", "tp"), None, None),
        check_vma=False,
    )
```

```python
import functools

import jax
import jax.numpy as jnp
from jax import lax
from jax.experimental import pallas as pl
from jax.experimental.pallas import tpu as pltpu
from jax.sharding import PartitionSpec as P

decay_scale = 8.0
norm_eps = 1e-05

pair_stages = 4
group_count = 4
taps = 4


def stages_of(planes):
    paired = 2 * pair_stages
    return pair_stages + (planes - paired) // 4


def plane_of(stage, group, side):
    if stage < pair_stages:
        return 2 * stage + side
    return 2 * pair_stages + 4 * (stage - pair_stages) + 2 * (group % 2) + side


def section(x, weights, vector, at):
    rows, width = x.shape
    length = at.shape[1]
    count = rows // length
    parts, _, chans = weights.shape
    depth = width // parts
    half = chans // 2
    proj = jnp.dot(x[:, :depth], weights[0, :depth, :], preferred_element_type=jnp.float32)
    for t in range(1, parts):
        proj = proj + jnp.dot(
            x[:, t * depth : (t + 1) * depth],
            weights[t, :depth, :],
            preferred_element_type=jnp.float32,
        )
    proj = proj.astype(jnp.bfloat16).astype(jnp.float32).reshape(count, length, chans)
    conv = vector[taps : taps + 1][None] + proj * vector[taps - 1 : taps][None]
    for back in range(1, taps):
        moved = jnp.where(at >= back, pltpu.roll(proj, back, axis=1), 0.0)
        conv = conv + moved * vector[taps - 1 - back : taps - back][None]
    flat = conv.astype(jnp.bfloat16).reshape(rows, chans)
    rate, gate = [], []
    for h in range(2):
        maps = jnp.concatenate(
            [weights[t, 2 * depth :, :] for t in range(h * parts // 2, (h + 1) * parts // 2)], axis=0
        )
        both = jnp.dot(
            flat[:, h * half : (h + 1) * half], maps, preferred_element_type=jnp.float32
        )
        rate.append(both[:, :half])
        gate.append(both[:, half:])
    rate = jnp.concatenate(rate, axis=1) + vector[5:6]
    gate = jnp.concatenate(gate, axis=1) + vector[6:7]
    rate = 1.0 / (1.0 + jnp.exp(-rate))
    gate = 1.0 / (1.0 + jnp.exp(-gate))
    log_decay = rate * vector[7:8]
    lost = 1.0 + log_decay * (1.0 / 7.0)
    for k in (6.0, 5.0, 4.0, 3.0, 2.0):
        lost = 1.0 + log_decay * (1.0 / k) * lost
    lost = lost * log_decay
    hidden = jnp.sqrt(-lost * (2.0 + lost)) * gate * flat.astype(jnp.float32)
    decay = (1.0 + lost).reshape(count, length, chans)
    hidden = hidden.reshape(count, length, chans)
    back = 1
    while back < length:
        hidden = hidden + decay * jnp.where(at >= back, pltpu.roll(hidden, back, axis=1), 0.0)
        if 2 * back < length:
            decay = decay * jnp.where(at >= back, pltpu.roll(decay, back, axis=1), 1.0)
        back = 2 * back
    mixed = hidden.astype(jnp.bfloat16).reshape(rows, chans)
    update = [
        jnp.dot(mixed[:, :half], weights[t, depth : 2 * depth, :half], preferred_element_type=jnp.float32)
        + jnp.dot(mixed[:, half:], weights[t, depth : 2 * depth, half:], preferred_element_type=jnp.float32)
        for t in range(parts)
    ]
    summed = x.astype(jnp.float32) + jnp.concatenate(update, axis=1)
    mean_value = jnp.mean(summed, axis=1, keepdims=True)
    centered = summed - mean_value
    variance = jnp.mean(centered * centered, axis=1, keepdims=True)
    lines = width // chans
    gain = jnp.concatenate([vector[8 + q : 9 + q] for q in range(lines)], axis=1)
    shift = jnp.concatenate([vector[8 + lines + q : 9 + lines + q] for q in range(lines)], axis=1)
    normed = centered * lax.rsqrt(variance + norm_eps) * gain + shift
    return normed.astype(jnp.bfloat16)


def stage_kernel(step, length, enters, x_ref, weights_ref, vectors_ref, *refs):
    o_ref = refs[-1]
    plane = lax.axis_index("pp")
    paired = 2 * pair_stages
    mine = lax.div(lax.rem(plane, 4), 2)
    in_pair = plane < paired
    stage = jnp.where(in_pair, lax.div(plane, 2), pair_stages + lax.div(plane - paired, 4))
    group = step - 2 * stage
    active = (group >= 0) & (group < group_count)
    active = active & (in_pair | (lax.rem(group + 2 * group_count, 2) == mine))
    first = jnp.where(in_pair, 2 * mine, 0)
    last = jnp.where(active, jnp.where(in_pair, 2 * mine + 2, 4), first)
    if enters:
        o_ref[...] = jnp.where(plane < 2, refs[0][...], x_ref[...])
    else:
        o_ref[...] = x_ref[...]
    rows = x_ref.shape[0]
    chans = vectors_ref.shape[2]
    at = lax.broadcasted_iota(jnp.int32, (rows // length, length, chans), 1)

    def one(j, unused):
        o_ref[...] = section(o_ref[...], weights_ref.at[:, j], vectors_ref[j], at)
        return unused

    lax.fori_loop(first, last, one, 0)


def run_stage(step, length, x, entry, weights, vectors):
    operands = (x, weights, vectors) + (() if entry is None else (entry,))
    rows, width = x.shape
    chans = vectors.shape[2]
    spec = pl.BlockSpec(memory_space=pltpu.VMEM)
    return pl.pallas_call(
        functools.partial(stage_kernel, step, length, entry is not None),
        out_shape=jax.ShapeDtypeStruct(x.shape, x.dtype),
        in_specs=[spec] * len(operands),
        out_specs=spec,
        compiler_params=pltpu.CompilerParams(vmem_limit_bytes=24 << 20),
        cost_estimate=pl.CostEstimate(
            flops=16 * rows * width * chans,
            bytes_accessed=16 * width * chans,
            transcendentals=20 * rows * chans,
        ),
        name="stage",
    )(*operands)


def flipped(place, by):
    if by == 1:
        return place + 1 - 2 * lax.rem(place, 2)
    return lax.rem(place + 2, 4) if by == 2 else 3 - place


def place_in_plane():
    part = lax.axis_index("tp")
    core = lax.rem(part, 2)
    colour = lax.rem(lax.div(part, 2) + 2 * lax.axis_index("fs"), 4)
    return colour, core


def join_kernel(flips, own, *refs):
    self_ref, ring_ref, mate_self_ref, mate_ring_ref = refs[:4]
    o_ref, done = refs[-2:]
    place = lax.rem(lax.axis_index("pp"), 4)
    colour, core = place_in_plane()
    lines = o_ref.shape[2]
    copies = []

    def put(source, target):
        copy = pltpu.make_async_copy(source, target, done.at[len(copies)])
        copy.start()
        copies.append(copy)

    if own:
        project_ref, back_ref, maps_ref = refs[4:7]
        depth = project_ref.shape[1]
        put(project_ref, o_ref.at[:, place, pl.ds(0, depth)])
        put(maps_ref, o_ref.at[:, place, pl.ds(2 * depth, lines - 2 * depth)])
        for t in range(o_ref.shape[0]):
            for h in range(2):
                put(
                    back_ref.at[pl.ds(h * depth, depth), pl.ds(t * depth, depth)],
                    o_ref.at[t, place, pl.ds(depth, depth), pl.ds(h * depth, depth)],
                )
    for i, by in enumerate(flips):
        slot = flipped(place, by)
        for side, alone, ring in ((core, self_ref, ring_ref), (1 - core, mate_self_ref, mate_ring_ref)):
            put(alone.at[i], o_ref.at[2 * colour + side, slot])
            for r, off in enumerate((3, 1, 2)):
                put(
                    ring.at[i, pl.ds(r * lines, lines)],
                    o_ref.at[2 * lax.rem(colour + off, 4) + side, slot],
                )
    for copy in copies:
        copy.wait()


def joined(flips, pieces, mine=None, stack=None):
    lines, chans = pieces[0].shape[1:]
    parts = mine[0].shape[0] if stack is None else stack.shape[0]
    whole = pl.BlockSpec(memory_space=pl.ANY)
    here = pl.BlockSpec(memory_space=pltpu.VMEM)
    count = 8 * len(flips) + (2 + 2 * parts if stack is None else 0)
    return pl.pallas_call(
        functools.partial(join_kernel, flips, stack is None),
        out_shape=jax.ShapeDtypeStruct((parts, 4, lines, chans), pieces[0].dtype),
        in_specs=[whole] * 7 if stack is None else [whole] * 4 + [here],
        out_specs=here,
        scratch_shapes=[pltpu.SemaphoreType.DMA((count,))],
        input_output_aliases={} if stack is None else {4: 0},
        compiler_params=pltpu.CompilerParams(vmem_limit_bytes=24 << 20),
        name="join",
    )(*pieces, *(mine if stack is None else (stack,)))


def block_maps(gate_rate, gate_input, parts):
    block = gate_rate.shape[1]
    place = jnp.arange(parts)[:, None] % (parts // 2) == jnp.arange(parts // 2)[None, :]
    maps = jnp.stack([gate_rate, gate_input], axis=2)[:, :, :, None, :]
    maps = jnp.where(place[:, None, None, :, None], maps, jnp.zeros((), maps.dtype))
    return maps.reshape(parts, block, parts * block)


def packed_shard(w_project, w_back, gate_rate, gate_input, parts):
    width, chans = w_project.shape
    depth, half, block = width // parts, chans // 2, gate_rate.shape[1]
    colour, core = place_in_plane()
    part = 2 * colour + core
    project = lax.dynamic_slice_in_dim(w_project, part * depth, depth, 0)
    back = lax.dynamic_slice_in_dim(w_back, part * depth, depth, 1)
    back = jnp.concatenate([back[:half], back[half:]], axis=1)
    maps = [lax.dynamic_index_in_dim(g, part, 0, keepdims=False) for g in (gate_rate, gate_input)]
    place = (jnp.arange(half) // block) == part % (parts // 2)
    maps = [jnp.where(place, jnp.tile(g, (1, half // block)), jnp.zeros((), g.dtype)) for g in maps]
    return jnp.concatenate([project, back, jnp.concatenate(maps, axis=1)], axis=0)


def shards(
    tokens_in,
    weight_in,
    conv_taps,
    conv_bias,
    gate_rate,
    bias_rate,
    gate_input,
    bias_input,
    decay_param,
    weight_out,
    norm_gain,
    norm_shift,
):
    planes = lax.axis_size("pp")
    parts = lax.axis_size("tp")
    splits = lax.axis_size("fs")
    plane = lax.axis_index("pp")
    length, width = tokens_in.shape[2:]
    chans = weight_in.shape[2]
    paired = 2 * pair_stages

    def moved(x, pairs):
        return lax.ppermute(x, "pp", [(int(a), int(b)) for a, b in pairs])

    place = plane % 4
    near_place = flipped(place, 1)

    def within(x, step_of, members):
        pairs = [
            ((z * splits + y) * parts + 2 * i + c, (z * splits + u) * parts + 2 * j + d)
            for z in members
            for y in range(splits)
            for i in range(parts // 2)
            for c in range(2)
            for u, j, d in [step_of(y, i, c)]
        ]
        return lax.ppermute(x, ("pp", "fs", "tp"), pairs)

    def from_neighbours(x, members):
        wide, lines = parts // 2, x.shape[1] // 2
        return [
            within(x, lambda y, i, c: (y, (i + 1) % wide, c), members),
            within(x, lambda y, i, c: (y, (i - 1) % wide, c), members),
            within(x[:, :lines], lambda y, i, c: ((y + 1) % splits, i, c), members),
            within(x[:, lines:], lambda y, i, c: ((y - 1) % splits, i, c), members),
        ]

    def from_mate(x, members):
        return within(x, lambda y, i, c: (y, i, 1 - c), members)

    project = weight_in.reshape(parts, width // parts, chans)
    maps = block_maps(gate_rate[0], gate_input[0], parts)
    shard = packed_shard(weight_in[0], weight_out[0], gate_rate[0], gate_input[0], parts)[None]
    swap = [(i, i ^ 1) for i in range(planes)]
    shard_near = moved(shard, swap)
    vector = jnp.concatenate(
        [
            conv_taps[0],
            conv_bias,
            bias_rate,
            bias_input,
            -decay_scale * jax.nn.softplus(-decay_param),
            norm_gain.reshape(-1, chans),
            norm_shift.reshape(-1, chans),
        ],
        axis=0,
    )[None]
    vector_near = moved(vector, swap)

    token = tokens_in.reshape(length, width)
    span = planes // group_count
    per = span // 2
    bases = [(g, s) for g in range(group_count) for s in range(2)]
    tokens = [
        moved(token, [(span * g + s + 2 * q, span * g + s) for g, s in bases]) for q in range(1, per)
    ]
    shard_near, *tokens = lax.optimization_barrier((shard_near, *tokens))
    collected = jnp.concatenate([token] + tokens, axis=0)
    entries = [
        moved(collected, [(span * g + s, s) for s in range(2)]) for g in range(1, group_count)
    ]

    everywhere, later = range(planes), range(paired, planes)
    across = [(i, i ^ 2) for i in later]
    far = moved(jnp.concatenate([shard, shard_near], axis=0), across)
    mate_self = from_mate(shard_near, everywhere)
    ring = jnp.concatenate(from_neighbours(shard_near, everywhere), axis=1)
    mate_ring = from_mate(ring, everywhere)
    vectors = jnp.zeros((4,) + vector.shape[1:], vector.dtype)
    vectors = lax.dynamic_update_slice_in_dim(vectors, vector, place, 0)
    vectors = lax.dynamic_update_slice_in_dim(vectors, vector_near, near_place, 0)
    far_vectors = moved(jnp.concatenate([vector, vector_near], axis=0), across)
    maps, vectors, collected, shard_near, ring, mate_self, mate_ring, *entries = (
        lax.optimization_barrier(
            (maps, vectors, collected, shard_near, ring, mate_self, mate_ring, *entries)
        )
    )
    entries = [collected] + entries
    weights = joined((1,), (shard_near, ring, mate_self, mate_ring), mine=(project, weight_out[0], maps))

    stages = stages_of(planes)
    outputs, arrived = [], []
    for step in range(2 * stages + group_count - 2):
        x = arrived[step - 2] if step >= 2 else None
        entry = entries[step] if step < group_count else None
        if x is None:
            x, entry = entry, None
        if step == 1:
            x = lax.optimization_barrier((x, outputs[0]))[0]
        y = run_stage(step, length, x, entry, weights, vectors)
        pairs = [
            (plane_of(i, step - 2 * i, s), plane_of(i + 1, step - 2 * i, s))
            for i in range(stages - 1)
            if 0 <= step - 2 * i < group_count
            for s in range(2)
        ]
        arrived.append(moved(y, pairs) if pairs else None)
        outputs.append(y)
        if step == 3:
            far, far_vectors, *_ = lax.optimization_barrier((far, far_vectors, y, arrived[2]))
            far_mate = from_mate(far, later)
            far_ring = from_neighbours(far, later)
        if step == 5:
            far_mate, *far_ring, _, _ = lax.optimization_barrier(
                (far_mate, *far_ring, y, arrived[4])
            )
            far_ring = jnp.concatenate(far_ring, axis=1)
            far_mate_ring = from_mate(far_ring, later)
            vectors_late = vectors
            for by, row in ((2, 0), (3, 1)):
                vectors_late = lax.dynamic_update_slice_in_dim(
                    vectors_late, far_vectors[row : row + 1], flipped(place, by), 0
                )
        if step == 2 * pair_stages - 2:
            far_mate_ring, vectors_late, _ = lax.optimization_barrier(
                (far_mate_ring, vectors_late, y)
            )
        if step == 2 * pair_stages - 1:
            weights = joined(
                (2, 3), (far, far_ring, far_mate, far_mate_ring), stack=weights
            )
            vectors = vectors_late

    last = stages - 1
    stay = [plane_of(last, group_count - 1, s) for s in range(2)]
    done = outputs[-1]
    early = None
    parts_in = [
        moved(outputs[2 * last + g], [(plane_of(last, g, s), span * g + s) for s in range(2)])
        for g in range(group_count - 1)
    ]
    parts_in, done = lax.optimization_barrier((parts_in, done))
    for part in parts_in:
        early = part if early is None else early + part
    at_end = plane >= stay[0]
    done = jnp.where(at_end, done, early).reshape(per, length, width)
    final = None
    for c in range(1, per):
        send = jnp.where(at_end, done[c - 1], done[c])
        pairs = [
            (span * g + s, span * g + s + 2 * c) for g in range(group_count - 1) for s in range(2)
        ] + [(stay[s], span * (group_count - 1) + s + 2 * (c - 1)) for s in range(2)]
        part = moved(send, pairs)
        final = part if final is None else final + part
    keeps = at_end | ((plane % span < 2) & (plane < span * (group_count - 1)))
    final = jnp.where(keeps, jnp.where(at_end, done[per - 1], done[0]), final)
    return final.reshape(1, 1, length, width)


def solution(mesh):
    placed = (
        P("pp", ("fs", "tp"), None, None),
        P("pp", None, None),
        P("pp", None, None),
        P("pp", None),
        P("pp", None, None, None),
        P("pp", None),
        P("pp", None, None, None),
        P("pp", None),
        P("pp", None),
        P("pp", None, None),
        P("pp", None),
        P("pp", None),
    )
    return jax.shard_map(
        shards,
        mesh=mesh,
        in_specs=placed,
        out_specs=P("pp", ("fs", "tp"), None, None),
        check_vma=False,
    )
```
